32 devices in a mesh: sp: 8 (over z, y), tp: 4 (over x, core).
Axes of the slice: x: 2, y: 2, z: 4, core: 2. Of those that a mesh axis runs over, the one named last changes fastest.
Arguments:
- tokens: bfloat16 [6144, 2048], P(('sp', 'tp')), may hold values from -6 to 6
- norm_gain: float32 [2048], replicated, may hold values from 0.1 to 1.9
- w_query: bfloat16 [2048, 1024], P('sp', 'tp'), may hold values from -0.125 to 0.125
- w_forget: bfloat16 [2048, 1024], P('sp', 'tp'), may hold values from -0.125 to 0.125
- w_input: bfloat16 [2048, 1024], P('sp', 'tp'), may hold values from -0.125 to 0.125
- w_outgate: bfloat16 [2048, 1024], P('sp', 'tp'), may hold values from -0.125 to 0.125
- w_conv_value: bfloat16 [2048, 1024], P('sp', 'tp'), may hold values from -0.125 to 0.125
- w_conv_gate: bfloat16 [2048, 1024], P('sp', 'tp'), may hold values from -0.125 to 0.125
- w_gate_rec: bfloat16 [2048, 2048], P('sp', 'tp'), may hold values from -0.125 to 0.125
- w_gate_conv: bfloat16 [2048, 2048], P('sp', 'tp'), may hold values from -0.125 to 0.125
- lower_bound: float32 [1024], P('tp'), may hold values from 0.92 to 0.99991862, as said below
- decay_shift: float32 [6144, 1024], P('sp', 'tp'), may hold values from -0.7 to 0, as said below
- state_init: float32 [8, 128, 128], P('tp'), may hold values from -0.1875 to 0.1875
- head_gain: float32 [1024], P('tp'), may hold values from 0.1 to 1.9
- conv_kernel: float32 [31, 1024], P(None, 'tp'), may hold values from -7.5 to 7.5
- channel_gain: float32 [1024], P('tp'), may hold values from 0.1 to 1.9
- channel_bias: float32 [1024], P('tp'), may hold values from -3 to 3
- w_out_rec: bfloat16 [1024, 2048], P('tp', 'sp'), may hold values from -0.1875 to 0.1875
- w_out_conv: bfloat16 [1024, 2048], P('tp', 'sp'), may hold values from -0.1875 to 0.1875
Outputs:
- mixed_out: bfloat16 [6144, 2048], P('sp', 'tp')
The draws below stay inside these ranges and needn't reach their ends.
Inputs may be any that keep to these rules, and one draw needn't show every extreme that they name: `lower_bound`: every entry is below one. `decay_shift`: no entry is positive.
All inputs are finite; a program needn't handle non-finite values.
Results may differ from the reference program's by a relative error of at most 0.017.
Values may be sent and summed in bfloat16 or wider, within the bound.
A program may use at most 64 MiB of HBM per device.

```python
import math
import jax
import jax.numpy as jnp
from jax import lax

D = 2048
HEADS = 8
HEAD = 128
CONV = 1024
KW = 31
BLOCK = 64
T_DEV = 768
HD = 1024
TOKENS = 6144


def draw_lower_bound(key, part):
    base_key = jax.random.fold_in(key, 11)
    head_key, slow_key, quick_seed = jax.random.split(base_key, 3)
    share = 0.5
    slow_heads = jax.random.uniform(head_key, (HEADS,), jnp.float32) < share
    slow_rate = jnp.exp(jax.random.uniform(slow_key, (HEADS, HEAD), jnp.float32, math.log(0.5), math.log(1.5))) / TOKENS
    fast_rate = jnp.exp(jax.random.uniform(quick_seed, (HEADS, HEAD), jnp.float32, math.log(0.03), math.log(0.08)))
    rate = jnp.where(slow_heads[:, None], slow_rate, fast_rate)
    return (1.0 - rate).reshape(HEADS * HEAD).astype(jnp.float32)


def draw_decay_shift(key, part):
    base_key = jax.random.fold_in(key, 23)
    block_key, position_key, depth_key = jax.random.split(base_key, 3)
    block_rate = jnp.exp(jax.random.uniform(block_key, (TOKENS // T_DEV,), jnp.float32, math.log(0.2), math.log(1.6)))
    starting_index = -jnp.repeat(block_rate, T_DEV) / TOKENS
    spots = jax.random.randint(position_key, (HEADS, 2), 0, TOKENS)
    places = jnp.arange(TOKENS, dtype=jnp.int32)
    dropped_sequence_items = jnp.any(places[:, None, None] == spots[None, :, :], axis=-1)
    memory_dimension = jax.random.uniform(depth_key, (TOKENS, HEADS, HEAD), jnp.float32, 0.22, 0.69)
    segment_span = jnp.where(dropped_sequence_items[:, :, None], -memory_dimension, 0.0)
    overall_aggregate = starting_index[:, None, None] + segment_span
    return overall_aggregate.reshape(TOKENS, HEADS * HEAD).astype(jnp.float32)


def draw_conv_kernel(key, part):
    base_key = jax.random.fold_in(key, 37)
    value_key = jax.random.fold_in(base_key, 0)
    rising = jnp.exp(math.log(6.0) * jnp.arange(CONV, dtype=jnp.float32) / CONV)
    entries = jnp.clip(jax.random.normal(value_key, (KW, CONV), jnp.float32), -4.0, 4.0)
    return (entries * rising / math.sqrt(KW)).astype(jnp.float32)


def block_levels(stream_key, dims, cuts, low, high):
    factor_of = 1.0
    for axis_at, parts in cuts:
        heights = jax.random.uniform(jax.random.fold_in(jax.random.fold_in(stream_key, 6), axis_at), (parts,), jnp.float32, low / len(cuts), high / len(cuts))
        factor_of = factor_of * jnp.repeat(jnp.exp(heights), dims[axis_at] // parts).reshape((-1,) + (1,) * (len(dims) - 1 - axis_at))
    return factor_of


def centred(key, dims, deviation, most, pieces=(), kind=jnp.bfloat16):
    values = deviation * jax.random.normal(key, dims, jnp.float32)
    if pieces:
        values = values * block_levels(key, dims, pieces, -0.22, 0.18)
    return jnp.clip(values, -most, most).astype(kind)


def setup_inputs(seed: int = 0) -> dict:
    key_of = jax.random.split(jax.random.key(seed), 20)
    tokens = centred(key_of[0], (TOKENS, D), 1.0, 6.0, ((0, 32),))
    norm_gain = jnp.clip(1.0 + 0.18 * jax.random.normal(key_of[1], (D,), jnp.float32), 0.1, 1.9)
    w_query = centred(key_of[2], (D, HD), D ** -0.5, 0.125, ((0, 8), (1, 4)))
    w_forget = centred(key_of[3], (D, HD), D ** -0.5, 0.125, ((0, 8), (1, 4)))
    w_input = centred(key_of[4], (D, HD), D ** -0.5, 0.125, ((0, 8), (1, 4)))
    w_outgate = centred(key_of[5], (D, HD), D ** -0.5, 0.125, ((0, 8), (1, 4)))
    w_conv_value = centred(key_of[6], (D, CONV), D ** -0.5, 0.125, ((0, 8), (1, 4)))
    w_conv_gate = centred(key_of[7], (D, CONV), D ** -0.5, 0.125, ((0, 8), (1, 4)))
    w_gate_rec = centred(key_of[8], (D, D), D ** -0.5, 0.125, ((0, 8), (1, 4)))
    w_gate_conv = centred(key_of[9], (D, D), D ** -0.5, 0.125, ((0, 8), (1, 4)))
    lower_bound = draw_lower_bound(jax.random.fold_in(key_of[19], 71), 0)
    decay_shift = draw_decay_shift(jax.random.fold_in(key_of[19], 71), 0)
    state_init = centred(key_of[12], (HEADS, HEAD, HEAD), (TOKENS ** -0.5), 0.1875, ((0, 4),), jnp.float32)
    head_gain = jnp.clip(1.0 + 0.18 * jax.random.normal(key_of[13], (HD,), jnp.float32), 0.1, 1.9)
    conv_kernel = draw_conv_kernel(jax.random.fold_in(key_of[19], 71), 0)
    channel_gain = jnp.clip(1.0 + 0.18 * jax.random.normal(key_of[15], (CONV,), jnp.float32), 0.1, 1.9)
    channel_bias = centred(key_of[16], (CONV,), 0.5, 3.0, ((0, 4),), jnp.float32)
    w_out_rec = centred(key_of[17], (HD, D), HD ** -0.5, 0.1875, ((0, 4), (1, 8)))
    w_out_conv = centred(key_of[18], (CONV, D), CONV ** -0.5, 0.1875, ((0, 4), (1, 8)))
    return dict(tokens=tokens, norm_gain=norm_gain, w_query=w_query, w_forget=w_forget, w_input=w_input, w_outgate=w_outgate, w_conv_value=w_conv_value, w_conv_gate=w_conv_gate, w_gate_rec=w_gate_rec, w_gate_conv=w_gate_conv, lower_bound=lower_bound, decay_shift=decay_shift, state_init=state_init, head_gain=head_gain, conv_kernel=conv_kernel, channel_gain=channel_gain, channel_bias=channel_bias, w_out_rec=w_out_rec, w_out_conv=w_out_conv)


EPSILON = 1e-06
highest_precision = lax.Precision.HIGHEST

def normalize_rows(values, gain_vector):
    widened = values.astype(jnp.float32)
    scale = lax.rsqrt(lax.optimization_barrier(jnp.mean(widened * widened, axis=-1, keepdims=True)) + EPSILON)
    return (widened * scale * gain_vector).astype(jnp.bfloat16)

def block_step(state, inputs):
    query, input_gate, values, log_decay = inputs
    length = query.shape[1]
    causal_masked = (jnp.arange(length)[:, None] >= jnp.arange(length)[None, :])[None, :, :, None]
    cumulative = jnp.cumsum(log_decay, axis=1)
    spread = cumulative[:, :, None, :] - cumulative[:, None, :, :]
    weight = jnp.where(causal_masked, jnp.exp(jnp.where(causal_masked, spread, 0.0)), 0.0)
    scores = jnp.einsum('htd,hsd,htsd->hts', query, input_gate, weight, precision=highest_precision)
    output = jnp.einsum('hts,hsv->htv', scores, values, precision=highest_precision)
    output = output + jnp.einsum('htd,hdv->htv', query * jnp.exp(cumulative), state, precision=highest_precision)
    final = cumulative[:, -1:, :]
    carried = jnp.exp(final[:, 0, :])[:, :, None] * state
    carried = carried + jnp.einsum('hsd,hsv->hdv', input_gate * jnp.exp(final - cumulative), values, precision=highest_precision)
    return (carried, output)

def reference(tokens, norm_gain, w_query, w_forget, w_input, w_outgate, w_conv_value, w_conv_gate, w_gate_rec, w_gate_conv, lower_bound, decay_shift, state_init, head_gain, conv_kernel, channel_gain, channel_bias, w_out_rec, w_out_conv):
    normed = normalize_rows(tokens, norm_gain)

    def project(weight):
        return jnp.dot(normed, weight, preferred_element_type=jnp.float32).astype(jnp.bfloat16)
    query_raw = project(w_query)
    forget_raw = project(w_forget)
    input_raw = project(w_input)
    outgate_raw = project(w_outgate)
    value_raw = project(w_conv_value)
    gate_raw = project(w_conv_gate)
    gate_rec_raw = project(w_gate_rec)
    gate_conv_raw = project(w_gate_conv)
    query = jax.nn.silu(query_raw.astype(jnp.float32))
    input_gate = (1.0 - lower_bound) * jax.nn.sigmoid(-forget_raw.astype(jnp.float32))
    log_decay = jnp.log1p(-input_gate) + decay_shift
    values = input_raw.astype(jnp.float32)
    block_count = TOKENS // BLOCK

    def to_blocks(array):
        return array.reshape(block_count, BLOCK, HEADS, HEAD).transpose(0, 2, 1, 3)
    unused_state, blocks_out = lax.scan(block_step, state_init, (to_blocks(query), to_blocks(input_gate), to_blocks(values), to_blocks(log_decay)))
    head_out = blocks_out.transpose(0, 2, 1, 3).reshape(TOKENS, HEADS, HEAD)
    head_out = head_out * lax.rsqrt(lax.optimization_barrier(jnp.mean(head_out * head_out, axis=-1, keepdims=True)) + EPSILON)
    head_out = head_out * head_gain.reshape(HEADS, HEAD)
    mixed_rec = (head_out.reshape(TOKENS, HEADS * HEAD) * jax.nn.silu(outgate_raw.astype(jnp.float32))).astype(jnp.bfloat16)
    gated = (value_raw.astype(jnp.float32) * jax.nn.sigmoid(gate_raw.astype(jnp.float32))).astype(jnp.bfloat16)
    extended = jnp.concatenate([jnp.zeros((KW - 1, CONV), jnp.bfloat16), gated], axis=0).astype(jnp.float32)
    conv_out = jnp.zeros((TOKENS, CONV), jnp.float32)
    for tap_index in range(KW):
        conv_out = conv_out + conv_kernel[tap_index] * extended[tap_index:tap_index + TOKENS]
    scale = lax.rsqrt(lax.optimization_barrier(jnp.mean(conv_out * conv_out, axis=1, keepdims=True)) + EPSILON)
    mixed_conv = jax.nn.silu(conv_out * scale * channel_gain + channel_bias).astype(jnp.bfloat16)
    y_rec = jnp.dot(mixed_rec, w_out_rec, preferred_element_type=jnp.float32).astype(jnp.bfloat16)
    y_conv = jnp.dot(mixed_conv, w_out_conv, preferred_element_type=jnp.float32).astype(jnp.bfloat16)
    merged = jax.nn.sigmoid(gate_rec_raw.astype(jnp.float32)) * y_rec.astype(jnp.float32)
    merged = merged + jax.nn.sigmoid(gate_conv_raw.astype(jnp.float32)) * y_conv.astype(jnp.float32)
    return merged.astype(jnp.bfloat16)
```

```python
import functools

import jax
import jax.numpy as jnp
from jax import lax
from jax.experimental import pallas as pl
from jax.experimental.pallas import tpu as pltpu
from jax.sharding import PartitionSpec as P

HEAD = 128
CONV = 1024
KW = 31
BLOCK = 64
EPSILON = 1e-06
MESH = pl.DeviceIdType.MESH


def passed_along(block, axis, distance):
    devices = range(lax.axis_size(axis))
    route = [(i - distance, i) for i in devices if i - distance in devices]
    return lax.ppermute(block, axis, route)


def normalize_rows(values, gain_vector):
    widened = values.astype(jnp.float32)
    scale = lax.rsqrt(jnp.mean(widened * widened, axis=-1, keepdims=True) + EPSILON)
    return (widened * scale * gain_vector).astype(jnp.bfloat16)


def tp_partners(m):
    me = lax.axis_index("tp")
    core = me % 2
    chip = me // 2
    chips = m // 2
    others = [((chip + k) % chips) * 2 + core for k in range(1, chips)]
    sources = [((chip + chips - k) % chips) * 2 + core for k in range(1, chips)]
    sibling = chip * 2 + (1 - core)
    return me, others, sources, sibling


def remote(src, dst, send, recv, device):
    return pltpu.make_async_remote_copy(
        src_ref=src, dst_ref=dst, send_sem=send, recv_sem=recv, device_id=device, device_id_type=MESH
    )


def tp_start(own, out, m, send, recv, local_sem):
    me, others, sources, sibling = tp_partners(m)
    mine = pltpu.make_async_copy(own, out.at[me], local_sem)
    mine.start()
    started = []
    for k, other in enumerate(others):
        copy = remote(own, out.at[me], send.at[k], recv.at[k], {"tp": other})
        copy.start()
        started.append(copy)
    near = remote(own, out.at[me], send.at[m - 1], recv.at[m - 1], {"tp": sibling})
    near.start()
    return mine, started, near


def tp_forward(own, out, m, send, recv, state):
    mine, started, near = state
    me, others, sources, sibling = tp_partners(m)
    chips = m // 2
    handed = []
    for k, source in enumerate(sources):
        started[k].wait_recv()
        copy = remote(
            out.at[source],
            out.at[source],
            send.at[chips - 1 + k],
            recv.at[chips - 1 + k],
            {"tp": sibling},
        )
        copy.start()
        handed.append(copy)
    return mine, started, near, handed


def tp_finish(state):
    mine, started, near, handed = state
    for copy in started:
        copy.wait_send()
    near.wait()
    for copy in handed:
        copy.wait()
    mine.wait()


def greet(extra, m):
    me, others, sources, sibling = tp_partners(m)
    barrier = pltpu.get_barrier_semaphore()
    for other in others + [sibling]:
        pl.semaphore_signal(barrier, inc=1, device_id={"tp": other}, device_id_type=MESH)
    for device in extra:
        pl.semaphore_signal(barrier, inc=1, device_id={"sp": device}, device_id_type=MESH)
    pl.semaphore_wait(barrier, len(others) + 1 + len(extra))


def tp_gather_kernel(m, own, out, send, recv, local_sem):
    greet([], m)
    state = tp_start(own, out, m, send, recv, local_sem)
    tp_finish(tp_forward(own, out, m, send, recv, state))


def tp_gather(block, cid):
    m = lax.axis_size("tp")
    return pl.pallas_call(
        functools.partial(tp_gather_kernel, m),
        out_shape=jax.ShapeDtypeStruct((m,) + block.shape, block.dtype),
        in_specs=[pl.BlockSpec(memory_space=pl.ANY)],
        out_specs=pl.BlockSpec(memory_space=pl.ANY),
        scratch_shapes=[
            pltpu.SemaphoreType.DMA((m,)),
            pltpu.SemaphoreType.DMA((m,)),
            pltpu.SemaphoreType.DMA,
        ],
        compiler_params=pltpu.CompilerParams(collective_id=cid, has_side_effects=True),
    )(block)


def ring_kernel(n, m, w, tok, g, toks, wsend, wrecv, wlocal, tsend, trecv, tlocal):
    ny = n // 4 if n % 4 == 0 else 1
    nz = n // ny

    def place(index):
        z, y = index // ny, index % ny
        return y * nz + z + (y % 2) * (nz - 1 - 2 * z)

    def at(spot):
        spot = (spot + 2 * n) % n
        y, r = spot // nz, spot % nz
        return (r + (y % 2) * (nz - 1 - 2 * r)) * ny + y

    me = lax.axis_index("sp")
    pos = place(me)
    right, left = at(pos + 1), at(pos - 1)
    half = w.shape[0] // 2
    greet([right, left], m)
    mine = pltpu.make_async_copy(w, g.at[me], wlocal)
    mine.start()
    tstate = None
    copies = []
    for step in range(n - 1):
        for way, (device, sign) in enumerate(((right, -1), (left, 1))):
            rows = pl.ds(way * half, half)
            block = at(pos + sign * step)
            if step > 0:
                copies[2 * (step - 1) + way].wait_recv()
            copy = remote(
                w.at[rows] if step == 0 else g.at[block, rows],
                g.at[block, rows],
                wsend.at[step, way],
                wrecv.at[step, way],
                {"sp": device},
            )
            copy.start()
            copies.append(copy)
        if step == 0:
            tstate = tp_start(tok, toks, m, tsend, trecv, tlocal)
        if step == 2:
            tstate = tp_forward(tok, toks, m, tsend, trecv, tstate)
    for copy in copies[-2:]:
        copy.wait_recv()
    for copy in copies:
        copy.wait_send()
    mine.wait()
    tp_finish(tstate)


def ring_gather(w, tok):
    n, m = lax.axis_size("sp"), lax.axis_size("tp")
    return pl.pallas_call(
        functools.partial(ring_kernel, n, m),
        out_shape=(
            jax.ShapeDtypeStruct((n,) + w.shape, w.dtype),
            jax.ShapeDtypeStruct((m,) + tok.shape, tok.dtype),
        ),
        in_specs=[pl.BlockSpec(memory_space=pl.ANY)] * 2,
        out_specs=(pl.BlockSpec(memory_space=pl.ANY),) * 2,
        scratch_shapes=[
            pltpu.SemaphoreType.DMA((n - 1, 2)),
            pltpu.SemaphoreType.DMA((n - 1, 2)),
            pltpu.SemaphoreType.DMA,
            pltpu.SemaphoreType.DMA((m,)),
            pltpu.SemaphoreType.DMA((m,)),
            pltpu.SemaphoreType.DMA,
        ],
        compiler_params=pltpu.CompilerParams(collective_id=0, has_side_effects=True),
    )(w, tok)


def dot(a, b, dims):
    return lax.dot_general(a, b, (dims, ((), ())), preferred_element_type=jnp.float32)


def recurrence_kernel(q_ref, f_ref, i_ref, lb_ref, ds_ref, out_ref, qd_ref, st_ref, dec_ref):
    row = lax.broadcasted_iota(jnp.int32, (BLOCK, BLOCK), 0)
    col = lax.broadcasted_iota(jnp.int32, (BLOCK, BLOCK), 1)
    causal = row >= col
    lower = causal.astype(jnp.float32)
    slack = 1.0 - lb_ref[...]
    state = jnp.zeros((HEAD, HEAD), jnp.float32)
    run = jnp.zeros((1, HEAD), jnp.float32)
    for b in range(q_ref.shape[0] // BLOCK):
        rows = pl.ds(b * BLOCK, BLOCK)
        raw = q_ref[rows, :].astype(jnp.float32)
        query = raw * jax.nn.sigmoid(raw)
        gate = slack * jax.nn.sigmoid(-f_ref[rows, :].astype(jnp.float32))
        values = i_ref[rows, :]
        log_decay = jnp.log1p(-gate) + ds_ref[rows, :]
        cum = jnp.dot(
            lower, log_decay, precision=lax.Precision.HIGHEST, preferred_element_type=jnp.float32
        )
        final = cum[BLOCK - 1 :, :]
        qe = query * jnp.exp(cum)
        qb = qe.astype(jnp.bfloat16)
        ke = (gate * jnp.exp(-cum)).astype(jnp.bfloat16)
        scores = jnp.where(causal, dot(qb, ke, ((1,), (1,))), 0.0).astype(jnp.bfloat16)
        out = dot(scores, values, ((1,), (0,)))
        out_ref[rows, :] = out + dot(qb, state.astype(jnp.bfloat16), ((1,), (1,)))
        qd_ref[rows, :] = (qe * jnp.exp(run)).astype(jnp.bfloat16)
        kd = (gate * jnp.exp(final - cum)).astype(jnp.bfloat16)
        state = state * jnp.exp(final) + dot(values, kd, ((0,), (0,)))
        run = run + final
    st_ref[0] = state
    dec_ref[0] = jnp.exp(run)


def recurrence(raw, lower_bound, decay_shift, heads):
    rows = raw.shape[0]
    column = lambda k: pl.BlockSpec((rows, HEAD), lambda h: (0, k * heads + h))
    return pl.pallas_call(
        recurrence_kernel,
        grid=(heads,),
        out_shape=(
            jax.ShapeDtypeStruct((rows, heads * HEAD), jnp.float32),
            jax.ShapeDtypeStruct((rows, heads * HEAD), jnp.bfloat16),
            jax.ShapeDtypeStruct((heads, HEAD, HEAD), jnp.float32),
            jax.ShapeDtypeStruct((heads, 1, HEAD), jnp.float32),
        ),
        in_specs=[
            column(0),
            column(1),
            column(2),
            pl.BlockSpec((1, HEAD), lambda h: (0, h)),
            column(0),
        ],
        out_specs=(
            column(0),
            column(0),
            pl.BlockSpec((1, HEAD, HEAD), lambda h: (h, 0, 0)),
            pl.BlockSpec((1, 1, HEAD), lambda h: (h, 0, 0)),
        ),
    )(raw, raw, raw, lower_bound[None], decay_shift)


def local(
    tokens,
    norm_gain,
    w_query,
    w_forget,
    w_input,
    w_outgate,
    w_conv_value,
    w_conv_gate,
    w_gate_rec,
    w_gate_conv,
    lower_bound,
    decay_shift,
    state_init,
    head_gain,
    conv_kernel,
    channel_gain,
    channel_bias,
    w_out_rec,
    w_out_conv,
):
    n, m = lax.axis_size("sp"), lax.axis_size("tp")
    weights = (
        w_query,
        w_forget,
        w_input,
        w_outgate,
        w_conv_value,
        w_conv_gate,
        w_gate_rec,
        w_gate_conv,
        w_out_rec,
        w_out_conv,
    )
    width = w_query.shape[1]
    features = w_gate_rec.shape[1]
    gathered, rows_all = ring_gather(jnp.concatenate(weights, axis=1), tokens)
    inputs_width = 6 * width + 2 * features
    normed = normalize_rows(rows_all.reshape(-1, tokens.shape[1]), norm_gain)
    row_count = normed.shape[0]
    stacked = gathered.reshape(n * w_query.shape[0], -1)
    raw = jnp.dot(
        normed, stacked[:, :inputs_width], preferred_element_type=jnp.float32
    ).astype(jnp.bfloat16)
    out_w = gathered[:, :, inputs_width:].reshape(m, n // m, w_out_rec.shape[0], 2, -1)
    out_w = lax.all_to_all(out_w, "tp", split_axis=0, concat_axis=0, tiled=True)
    out_w = out_w.transpose(3, 0, 2, 1, 4).reshape(2, m * w_out_rec.shape[0], features)

    heads = width // HEAD
    local_out, decayed_query, local_state, forgetting = recurrence(
        raw, lower_bound, decay_shift, heads
    )
    states = lax.all_gather(local_state.astype(jnp.bfloat16), "sp").astype(jnp.float32)
    decays = lax.all_gather(forgetting.astype(jnp.bfloat16), "sp").astype(jnp.float32)
    position = lax.axis_index("sp")
    incoming = state_init.transpose(0, 2, 1)
    for k in range(n - 1):
        incoming = jnp.where(k < position, incoming * decays[k] + states[k], incoming)
    head_out = local_out.reshape(row_count, heads, HEAD) + jnp.einsum(
        "thd,hvd->thv",
        decayed_query.reshape(row_count, heads, HEAD),
        incoming.astype(jnp.bfloat16),
        preferred_element_type=jnp.float32,
    )
    head_out = head_out * lax.rsqrt(jnp.mean(head_out * head_out, axis=-1, keepdims=True) + EPSILON)
    head_out = head_out * head_gain.reshape(heads, HEAD)

    def part(k):
        return raw[:, k * width : (k + 1) * width].astype(jnp.float32)

    mixed_rec = (head_out.reshape(row_count, width) * jax.nn.silu(part(3))).astype(jnp.bfloat16)
    gated = (part(4) * jax.nn.sigmoid(part(5))).astype(jnp.bfloat16)
    rim_width = KW - 1
    previous = passed_along(gated[row_count - rim_width :], "sp", 1)
    extended = jnp.concatenate([previous, gated], axis=0).astype(jnp.float32)
    conv_out = jnp.zeros((row_count, width), jnp.float32)
    for tap_index in range(KW):
        conv_out = conv_out + conv_kernel[tap_index] * extended[tap_index : tap_index + row_count]
    squares = lax.psum(jnp.sum(conv_out * conv_out, axis=1), "tp")
    scale = lax.rsqrt(squares / CONV + EPSILON)[:, None]
    mixed_conv = jax.nn.silu(conv_out * scale * channel_gain + channel_bias).astype(jnp.bfloat16)

    both = tp_gather(jnp.concatenate([mixed_rec, mixed_conv], axis=1), 1)

    def project(branch):
        total = 0.0
        for t in range(m):
            total = total + jnp.dot(
                both[t, :, branch * width : (branch + 1) * width],
                out_w[branch, t * width : (t + 1) * width],
                preferred_element_type=jnp.float32,
            )
        return total.astype(jnp.bfloat16).astype(jnp.float32)

    gates = raw[:, 6 * width :].astype(jnp.float32)
    merged = jax.nn.sigmoid(gates[:, :features]) * project(0)
    merged = merged + jax.nn.sigmoid(gates[:, features:]) * project(1)
    return merged.astype(jnp.bfloat16)

def solution(mesh):
    in_specs = (
        P(("sp", "tp"), None),
        P(),
        P("sp", "tp"),
        P("sp", "tp"),
        P("sp", "tp"),
        P("sp", "tp"),
        P("sp", "tp"),
        P("sp", "tp"),
        P("sp", "tp"),
        P("sp", "tp"),
        P("tp"),
        P("sp", "tp"),
        P("tp", None, None),
        P("tp"),
        P(None, "tp"),
        P("tp"),
        P("tp"),
        P("tp", "sp"),
        P("tp", "sp"),
    )
    out_specs = P("sp", "tp")
    return jax.shard_map(local, mesh=mesh, in_specs=in_specs, out_specs=out_specs, check_vma=False)
```

```python
import functools

import jax
import jax.numpy as jnp
from jax import lax
from jax.experimental import pallas as pl
from jax.experimental.pallas import tpu as pltpu
from jax.sharding import PartitionSpec as P

HEAD = 128
CONV = 1024
KW = 31
BLOCK = 64
EPSILON = 1e-06
MESH = pl.DeviceIdType.MESH


def normalize_rows(values, gain_vector):
    widened = values.astype(jnp.float32)
    scale = lax.rsqrt(jnp.mean(widened * widened, axis=-1, keepdims=True) + EPSILON)
    return (widened * scale * gain_vector).astype(jnp.bfloat16)


def tp_partners(m):
    me = lax.axis_index("tp")
    core = me % 2
    chip = me // 2
    chips = m // 2
    others = [((chip + k) % chips) * 2 + core for k in range(1, chips)]
    sources = [((chip + chips - k) % chips) * 2 + core for k in range(1, chips)]
    sibling = chip * 2 + (1 - core)
    return me, others, sources, sibling


def remote(src, dst, send, recv, device):
    return pltpu.make_async_remote_copy(
        src_ref=src, dst_ref=dst, send_sem=send, recv_sem=recv, device_id=device, device_id_type=MESH
    )


def tp_start(own, out, m, send, recv, local_sem):
    me, others, sources, sibling = tp_partners(m)
    mine = pltpu.make_async_copy(own, out.at[me], local_sem)
    mine.start()
    started = []
    for k, other in enumerate(others):
        copy = remote(own, out.at[me], send.at[k], recv.at[k], {"tp": other})
        copy.start()
        started.append(copy)
    near = remote(own, out.at[me], send.at[m - 1], recv.at[m - 1], {"tp": sibling})
    near.start()
    return mine, started, near


def tp_forward(own, out, m, send, recv, state):
    mine, started, near = state
    me, others, sources, sibling = tp_partners(m)
    chips = m // 2
    handed = []
    for k, source in enumerate(sources):
        started[k].wait_recv()
        copy = remote(
            out.at[source],
            out.at[source],
            send.at[chips - 1 + k],
            recv.at[chips - 1 + k],
            {"tp": sibling},
        )
        copy.start()
        handed.append(copy)
    return mine, started, near, handed


def tp_finish(state):
    mine, started, near, handed = state
    for copy in started:
        copy.wait_send()
    near.wait()
    for copy in handed:
        copy.wait()
    mine.wait()


def greet(extra, m):
    me, others, sources, sibling = tp_partners(m)
    barrier = pltpu.get_barrier_semaphore()
    for other in others + [sibling]:
        pl.semaphore_signal(barrier, inc=1, device_id={"tp": other}, device_id_type=MESH)
    for device in extra:
        pl.semaphore_signal(barrier, inc=1, device_id={"sp": device}, device_id_type=MESH)
    pl.semaphore_wait(barrier, len(others) + 1 + len(extra))


def tp_gather_kernel(m, own, out, send, recv, local_sem):
    greet([], m)
    state = tp_start(own, out, m, send, recv, local_sem)
    tp_finish(tp_forward(own, out, m, send, recv, state))


def tp_gather(block, cid):
    m = lax.axis_size("tp")
    return pl.pallas_call(
        functools.partial(tp_gather_kernel, m),
        out_shape=jax.ShapeDtypeStruct((m,) + block.shape, block.dtype),
        in_specs=[pl.BlockSpec(memory_space=pl.ANY)],
        out_specs=pl.BlockSpec(memory_space=pl.ANY),
        scratch_shapes=[
            pltpu.SemaphoreType.DMA((m,)),
            pltpu.SemaphoreType.DMA((m,)),
            pltpu.SemaphoreType.DMA,
        ],
        compiler_params=pltpu.CompilerParams(collective_id=cid, has_side_effects=True),
    )(block)


def ring_kernel(
    n, m, first, w, tok, g, toks, ow, wsend, wrecv, wlocal, tsend, trecv, tlocal, osend, orecv
):
    ny = n // 4 if n % 4 == 0 else 1
    nz = n // ny

    def place(index):
        z, y = index // ny, index % ny
        return y * nz + z + (y % 2) * (nz - 1 - 2 * z)

    def at(spot):
        spot = (spot + 2 * n) % n
        y, r = spot // nz, spot % nz
        return (r + (y % 2) * (nz - 1 - 2 * r)) * ny + y

    me = lax.axis_index("sp")
    pos = place(me)
    right, left = at(pos + 1), at(pos - 1)
    half = w.shape[0] // 2
    tp = lax.axis_index("tp")
    share = n // m
    columns = pl.ds(first, w.shape[1] - first)
    handed = []

    def hand(block, way):
        owner, slot, rows = block // share, block % share, pl.ds(way * half, half)
        copy = remote(
            g.at[block, rows, columns],
            ow.at[tp, slot, rows],
            osend.at[len(handed)],
            orecv.at[tp, slot, way],
            {"tp": owner},
        )
        handed.append((owner, copy))

        @pl.when(owner != tp)
        def _():
            copy.start()

    greet_all([right, left], m)
    mine = pltpu.make_async_copy(w, g.at[me], wlocal)
    mine.start()
    tstate = None
    copies = []
    for step in range(n - 1):
        for way, (device, sign) in enumerate(((right, -1), (left, 1))):
            rows = pl.ds(way * half, half)
            block = at(pos + sign * step)
            if step > 0:
                copies[2 * (step - 1) + way].wait_recv()
            copy = remote(
                w.at[rows] if step == 0 else g.at[block, rows],
                g.at[block, rows],
                wsend.at[step, way],
                wrecv.at[step, way],
                {"sp": device},
            )
            copy.start()
            copies.append(copy)
            if step > 0:
                hand(block, way)
        if step == 0:
            tstate = tp_start(tok, toks, m, tsend, trecv, tlocal)
        if step == 2:
            tstate = tp_forward(tok, toks, m, tsend, trecv, tstate)
            mine.wait()
            for way in range(2):
                hand(me, way)
    for way, sign in enumerate((-1, 1)):
        copies[2 * (n - 2) + way].wait_recv()
        hand(at(pos + sign * (n - 1)), way)
    for copy in copies:
        copy.wait_send()
    tp_finish(tstate)
    for owner, copy in handed:

        @pl.when(owner != tp)
        def _(copy=copy):
            copy.wait_send()

    for k in range(1, m):
        source = (tp + k) % m
        for slot in range(share):
            for way in range(2):
                rows = pl.ds(way * half, half)
                landed = ow.at[source, slot, rows]
                remote(
                    landed, landed, osend.at[0], orecv.at[source, slot, way], {"tp": source}
                ).wait_recv()


def greet_all(extra, m):
    me = lax.axis_index("tp")
    barrier = pltpu.get_barrier_semaphore()
    for k in range(1, m):
        pl.semaphore_signal(
            barrier, inc=1, device_id={"tp": (me + k) % m}, device_id_type=MESH
        )
    for device in extra:
        pl.semaphore_signal(barrier, inc=1, device_id={"sp": device}, device_id_type=MESH)
    pl.semaphore_wait(barrier, m - 1 + len(extra))


def exchange_kernel(n, own, rim, out, before, send, recv, rsend, rrecv, local_sem):
    me = lax.axis_index("sp")
    barrier = pltpu.get_barrier_semaphore()
    for k in range(1, n):
        pl.semaphore_signal(
            barrier, inc=1, device_id={"sp": (me + k) % n}, device_id_type=MESH
        )
    mine = pltpu.make_async_copy(own, out.at[me], local_sem)
    mine.start()
    pl.semaphore_wait(barrier, n - 1)
    copies = [remote(rim, before, rsend, rrecv, {"sp": (me + 1) % n})]
    for k in range(1, n):
        copies.append(
            remote(own, out.at[me], send.at[k - 1], recv.at[k - 1], {"sp": (me + k) % n})
        )
    for copy in copies:
        copy.start()
    for copy in copies:
        copy.wait()
    mine.wait()


def exchange(own, rim):
    n = lax.axis_size("sp")
    return pl.pallas_call(
        functools.partial(exchange_kernel, n),
        out_shape=(
            jax.ShapeDtypeStruct((n,) + own.shape, own.dtype),
            jax.ShapeDtypeStruct(rim.shape, rim.dtype),
        ),
        in_specs=[pl.BlockSpec(memory_space=pl.ANY)] * 2,
        out_specs=(pl.BlockSpec(memory_space=pl.ANY),) * 2,
        scratch_shapes=[
            pltpu.SemaphoreType.DMA((n - 1,)),
            pltpu.SemaphoreType.DMA((n - 1,)),
            pltpu.SemaphoreType.DMA,
            pltpu.SemaphoreType.DMA,
            pltpu.SemaphoreType.DMA,
        ],
        compiler_params=pltpu.CompilerParams(collective_id=3, has_side_effects=True),
    )(own, rim)


def ring_gather(w, tok, first):
    n, m = lax.axis_size("sp"), lax.axis_size("tp")
    return pl.pallas_call(
        functools.partial(ring_kernel, n, m, first),
        out_shape=(
            jax.ShapeDtypeStruct((n,) + w.shape, w.dtype),
            jax.ShapeDtypeStruct((m,) + tok.shape, tok.dtype),
            jax.ShapeDtypeStruct((m, n // m, w.shape[0], w.shape[1] - first), w.dtype),
        ),
        in_specs=[pl.BlockSpec(memory_space=pl.ANY)] * 2,
        out_specs=(pl.BlockSpec(memory_space=pl.ANY),) * 3,
        scratch_shapes=[
            pltpu.SemaphoreType.DMA((n - 1, 2)),
            pltpu.SemaphoreType.DMA((n - 1, 2)),
            pltpu.SemaphoreType.DMA,
            pltpu.SemaphoreType.DMA((m,)),
            pltpu.SemaphoreType.DMA((m,)),
            pltpu.SemaphoreType.DMA,
            pltpu.SemaphoreType.DMA((2 * n,)),
            pltpu.SemaphoreType.DMA((m, n // m, 2)),
        ],
        compiler_params=pltpu.CompilerParams(collective_id=0, has_side_effects=True),
    )(w, tok)


def dot(a, b, dims):
    return lax.dot_general(a, b, (dims, ((), ())), preferred_element_type=jnp.float32)


def recurrence_kernel(q_ref, f_ref, i_ref, lb_ref, ds_ref, out_ref, qd_ref, st_ref, dec_ref):
    row = lax.broadcasted_iota(jnp.int32, (BLOCK, BLOCK), 0)
    col = lax.broadcasted_iota(jnp.int32, (BLOCK, BLOCK), 1)
    causal = row >= col
    lower = causal.astype(jnp.float32)
    slack = 1.0 - lb_ref[...]
    state = jnp.zeros((HEAD, HEAD), jnp.float32)
    run = jnp.zeros((1, HEAD), jnp.float32)
    for b in range(q_ref.shape[0] // BLOCK):
        rows = pl.ds(b * BLOCK, BLOCK)
        raw = q_ref[rows, :].astype(jnp.float32)
        query = raw * jax.nn.sigmoid(raw)
        gate = slack * jax.nn.sigmoid(-f_ref[rows, :].astype(jnp.float32))
        values = i_ref[rows, :]
        log_decay = jnp.log1p(-gate) + ds_ref[rows, :]
        cum = jnp.dot(
            lower, log_decay, precision=lax.Precision.HIGHEST, preferred_element_type=jnp.float32
        )
        final = cum[BLOCK - 1 :, :]
        qe = query * jnp.exp(cum)
        qb = qe.astype(jnp.bfloat16)
        ke = (gate * jnp.exp(-cum)).astype(jnp.bfloat16)
        scores = jnp.where(causal, dot(qb, ke, ((1,), (1,))), 0.0).astype(jnp.bfloat16)
        out = dot(scores, values, ((1,), (0,)))
        out_ref[rows, :] = out + dot(qb, state.astype(jnp.bfloat16), ((1,), (1,)))
        qd_ref[rows, :] = (qe * jnp.exp(run)).astype(jnp.bfloat16)
        kd = (gate * jnp.exp(final - cum)).astype(jnp.bfloat16)
        state = state * jnp.exp(final) + dot(values, kd, ((0,), (0,)))
        run = run + final
    st_ref[0] = state
    dec_ref[0] = jnp.exp(run)


def recurrence(raw, lower_bound, decay_shift, heads):
    rows = raw.shape[0]
    column = lambda k: pl.BlockSpec((rows, HEAD), lambda h: (0, k * heads + h))
    return pl.pallas_call(
        recurrence_kernel,
        grid=(heads,),
        out_shape=(
            jax.ShapeDtypeStruct((rows, heads * HEAD), jnp.float32),
            jax.ShapeDtypeStruct((rows, heads * HEAD), jnp.bfloat16),
            jax.ShapeDtypeStruct((heads, HEAD, HEAD), jnp.float32),
            jax.ShapeDtypeStruct((heads, 1, HEAD), jnp.float32),
        ),
        in_specs=[
            column(0),
            column(1),
            column(2),
            pl.BlockSpec((1, HEAD), lambda h: (0, h)),
            column(0),
        ],
        out_specs=(
            column(0),
            column(0),
            pl.BlockSpec((1, HEAD, HEAD), lambda h: (h, 0, 0)),
            pl.BlockSpec((1, 1, HEAD), lambda h: (h, 0, 0)),
        ),
    )(raw, raw, raw, lower_bound[None], decay_shift)


def local(
    tokens,
    norm_gain,
    w_query,
    w_forget,
    w_input,
    w_outgate,
    w_conv_value,
    w_conv_gate,
    w_gate_rec,
    w_gate_conv,
    lower_bound,
    decay_shift,
    state_init,
    head_gain,
    conv_kernel,
    channel_gain,
    channel_bias,
    w_out_rec,
    w_out_conv,
):
    n, m = lax.axis_size("sp"), lax.axis_size("tp")
    weights = (
        w_query,
        w_forget,
        w_input,
        w_outgate,
        w_conv_value,
        w_conv_gate,
        w_gate_rec,
        w_gate_conv,
        w_out_rec,
        w_out_conv,
    )
    width = w_query.shape[1]
    features = w_gate_rec.shape[1]
    inputs_width = 6 * width + 2 * features
    gathered, rows_all, out_w = ring_gather(
        jnp.concatenate(weights, axis=1), tokens, inputs_width
    )
    normed = normalize_rows(rows_all.reshape(-1, tokens.shape[1]), norm_gain)
    row_count = normed.shape[0]
    stacked = gathered.reshape(n * w_query.shape[0], -1)
    raw = jnp.dot(
        normed, stacked[:, :inputs_width], preferred_element_type=jnp.float32
    ).astype(jnp.bfloat16)
    share = n // m
    me = lax.axis_index("tp")
    own_w = lax.dynamic_slice_in_dim(gathered, me * share, share, 0)[:, :, inputs_width:]
    out_w = lax.dynamic_update_slice_in_dim(out_w, own_w[None], me, 0)
    out_rows, out_columns = w_out_rec.shape

    def part(k):
        return raw[:, k * width : (k + 1) * width].astype(jnp.float32)

    gated = (part(4) * jax.nn.sigmoid(part(5))).astype(jnp.bfloat16)

    heads = width // HEAD
    local_out, decayed_query, local_state, forgetting = recurrence(
        raw, lower_bound, decay_shift, heads
    )
    handover = jnp.concatenate(
        [local_state, jnp.broadcast_to(forgetting, (heads, 16, HEAD))], axis=1
    ).astype(jnp.bfloat16)
    rim_width = KW - 1
    everything, previous = exchange(handover, gated[row_count - 32 :])
    everything = everything.astype(jnp.float32)
    states, decays = everything[:, :, :HEAD], everything[:, :, HEAD : HEAD + 1]
    position = lax.axis_index("sp")
    previous = jnp.where(position > 0, previous[32 - rim_width :], 0)
    incoming = state_init.transpose(0, 2, 1)
    for k in range(n - 1):
        incoming = jnp.where(k < position, incoming * decays[k] + states[k], incoming)
    head_out = local_out.reshape(row_count, heads, HEAD) + jnp.einsum(
        "thd,hvd->thv",
        decayed_query.reshape(row_count, heads, HEAD),
        incoming.astype(jnp.bfloat16),
        preferred_element_type=jnp.float32,
    )
    head_out = head_out * lax.rsqrt(jnp.mean(head_out * head_out, axis=-1, keepdims=True) + EPSILON)
    head_out = head_out * head_gain.reshape(heads, HEAD)

    mixed_rec = (head_out.reshape(row_count, width) * jax.nn.silu(part(3))).astype(jnp.bfloat16)
    extended = jnp.concatenate([previous, gated], axis=0).astype(jnp.float32)
    conv_out = jnp.zeros((row_count, width), jnp.float32)
    for tap_index in range(KW):
        conv_out = conv_out + conv_kernel[tap_index] * extended[tap_index : tap_index + row_count]
    squares = tp_gather(jnp.sum(conv_out * conv_out, axis=1).reshape(-1, HEAD), 2)
    squares = jnp.sum(squares, axis=0).reshape(row_count)
    scale = lax.rsqrt(squares / CONV + EPSILON)[:, None]
    mixed_conv = jax.nn.silu(conv_out * scale * channel_gain + channel_bias).astype(jnp.bfloat16)

    both = tp_gather(jnp.concatenate([mixed_rec, mixed_conv], axis=1), 1)

    def project(branch):
        first = branch * out_columns
        blocks = []
        for j in range(share):
            total = 0.0
            for t in range(m):
                total = total + jnp.dot(
                    both[t, :, branch * width : (branch + 1) * width],
                    out_w[t, j, :, first : first + out_columns],
                    preferred_element_type=jnp.float32,
                )
            blocks.append(total.astype(jnp.bfloat16))
        return jnp.concatenate(blocks, axis=1).astype(jnp.float32)

    gates = raw[:, 6 * width :].astype(jnp.float32)
    merged = jax.nn.sigmoid(gates[:, :features]) * project(0)
    merged = merged + jax.nn.sigmoid(gates[:, features:]) * project(1)
    return merged.astype(jnp.bfloat16)

def solution(mesh):
    in_specs = (
        P(("sp", "tp"), None),
        P(),
        P("sp", "tp"),
        P("sp", "tp"),
        P("sp", "tp"),
        P("sp", "tp"),
        P("sp", "tp"),
        P("sp", "tp"),
        P("sp", "tp"),
        P("sp", "tp"),
        P("tp"),
        P("sp", "tp"),
        P("tp", None, None),
        P("tp"),
        P(None, "tp"),
        P("tp"),
        P("tp"),
        P("tp", "sp"),
        P("tp", "sp"),
    )
    out_specs = P("sp", "tp")
    return jax.shard_map(local, mesh=mesh, in_specs=in_specs, out_specs=out_specs, check_vma=False)
```

```python
import functools

import jax
import jax.numpy as jnp
from jax import lax
from jax.experimental import pallas as pl
from jax.experimental.pallas import tpu as pltpu
from jax.sharding import PartitionSpec as P

HEAD = 128
CONV = 1024
KW = 31
BLOCK = 64
EPSILON = 1e-06
MESH = pl.DeviceIdType.MESH


def normalize_rows(values, gain_vector):
    widened = values.astype(jnp.float32)
    scale = lax.rsqrt(jnp.mean(widened * widened, axis=-1, keepdims=True) + EPSILON)
    return (widened * scale * gain_vector).astype(jnp.bfloat16)


def tp_partners(m):
    me = lax.axis_index("tp")
    core = me % 2
    chip = me // 2
    chips = m // 2
    others = [((chip + k) % chips) * 2 + core for k in range(1, chips)]
    sources = [((chip + chips - k) % chips) * 2 + core for k in range(1, chips)]
    sibling = chip * 2 + (1 - core)
    return me, others, sources, sibling


def remote(src, dst, send, recv, device):
    return pltpu.make_async_remote_copy(
        src_ref=src, dst_ref=dst, send_sem=send, recv_sem=recv, device_id=device, device_id_type=MESH
    )


def tp_start(own, out, m, send, recv, local_sem):
    me, others, sources, sibling = tp_partners(m)
    mine = pltpu.make_async_copy(own, out.at[me], local_sem)
    mine.start()
    started = []
    for k, other in enumerate(others):
        copy = remote(own, out.at[me], send.at[k], recv.at[k], {"tp": other})
        copy.start()
        started.append(copy)
    near = remote(own, out.at[me], send.at[m - 1], recv.at[m - 1], {"tp": sibling})
    near.start()
    return mine, started, near


def tp_forward(own, out, m, send, recv, state):
    mine, started, near = state
    me, others, sources, sibling = tp_partners(m)
    chips = m // 2
    handed = []
    for k, source in enumerate(sources):
        started[k].wait_recv()
        copy = remote(
            out.at[source],
            out.at[source],
            send.at[chips - 1 + k],
            recv.at[chips - 1 + k],
            {"tp": sibling},
        )
        copy.start()
        handed.append(copy)
    return mine, started, near, handed


def tp_finish(state):
    mine, started, near, handed = state
    for copy in started:
        copy.wait_send()
    near.wait()
    for copy in handed:
        copy.wait()
    mine.wait()


def greet(extra, m):
    me, others, sources, sibling = tp_partners(m)
    barrier = pltpu.get_barrier_semaphore()
    for other in others + [sibling]:
        pl.semaphore_signal(barrier, inc=1, device_id={"tp": other}, device_id_type=MESH)
    for device in extra:
        pl.semaphore_signal(barrier, inc=1, device_id={"sp": device}, device_id_type=MESH)
    pl.semaphore_wait(barrier, len(others) + 1 + len(extra))


def tp_gather_kernel(m, pieces, own, out, send, recv, local_sem):
    greet([], m)
    size = own.shape[0] // pieces
    views = []
    for c in range(pieces):
        rows = pl.ds(c * size, size)
        views.append((own.at[rows], out.at[:, rows], m, send.at[c], recv.at[c]))
    states = [tp_start(*view, local_sem.at[c]) for c, view in enumerate(views)]
    states = [tp_forward(*view, state) for view, state in zip(views, states)]
    for state in states:
        tp_finish(state)


def tp_gather(block, cid, pieces=1):
    m = lax.axis_size("tp")
    return pl.pallas_call(
        functools.partial(tp_gather_kernel, m, pieces),
        out_shape=jax.ShapeDtypeStruct((m,) + block.shape, block.dtype),
        in_specs=[pl.BlockSpec(memory_space=pl.ANY)],
        out_specs=pl.BlockSpec(memory_space=pl.ANY),
        scratch_shapes=[
            pltpu.SemaphoreType.DMA((pieces, m)),
            pltpu.SemaphoreType.DMA((pieces, m)),
            pltpu.SemaphoreType.DMA((pieces,)),
        ],
        compiler_params=pltpu.CompilerParams(collective_id=cid, has_side_effects=True),
    )(block)


def ring_kernel(
    n, m, first, w, tok, g, toks, ow, wsend, wrecv, wlocal, tsend, trecv, tlocal, osend, orecv
):
    ny = n // 4 if n % 4 == 0 else 1
    nz = n // ny

    def place(index):
        z, y = index // ny, index % ny
        return y * nz + z + (y % 2) * (nz - 1 - 2 * z)

    def at(spot):
        spot = (spot + 2 * n) % n
        y, r = spot // nz, spot % nz
        return (r + (y % 2) * (nz - 1 - 2 * r)) * ny + y

    me = lax.axis_index("sp")
    pos = place(me)
    right, left = at(pos + 1), at(pos - 1)
    half = w.shape[0] // 2
    tp = lax.axis_index("tp")
    share = n // m
    columns = pl.ds(first, w.shape[1] - first)
    handed = []

    def hand(block, way):
        owner, slot, rows = block // share, block % share, pl.ds(way * half, half)
        copy = remote(
            g.at[block, rows, columns],
            ow.at[tp, slot, rows],
            osend.at[len(handed)],
            orecv.at[tp, slot, way],
            {"tp": owner},
        )
        handed.append((owner, copy))

        @pl.when(owner != tp)
        def _():
            copy.start()

    greet_all([right, left], m)
    mine = pltpu.make_async_copy(w, g.at[me], wlocal)
    mine.start()
    tstate = None
    copies = []
    for step in range(n - 1):
        for way, (device, sign) in enumerate(((right, -1), (left, 1))):
            rows = pl.ds(way * half, half)
            block = at(pos + sign * step)
            if step > 0:
                copies[2 * (step - 1) + way].wait_recv()
            copy = remote(
                w.at[rows] if step == 0 else g.at[block, rows],
                g.at[block, rows],
                wsend.at[step, way],
                wrecv.at[step, way],
                {"sp": device},
            )
            copy.start()
            copies.append(copy)
            if step > 0:
                hand(block, way)
        if step == 0:
            tstate = tp_start(tok, toks, m, tsend, trecv, tlocal)
        if step == 2:
            tstate = tp_forward(tok, toks, m, tsend, trecv, tstate)
            mine.wait()
            for way in range(2):
                hand(me, way)
    for way, sign in enumerate((-1, 1)):
        copies[2 * (n - 2) + way].wait_recv()
        hand(at(pos + sign * (n - 1)), way)
    for copy in copies:
        copy.wait_send()
    tp_finish(tstate)
    for owner, copy in handed:

        @pl.when(owner != tp)
        def _(copy=copy):
            copy.wait_send()

    for k in range(1, m):
        source = (tp + k) % m
        for slot in range(share):
            for way in range(2):
                rows = pl.ds(way * half, half)
                landed = ow.at[source, slot, rows]
                remote(
                    landed, landed, osend.at[0], orecv.at[source, slot, way], {"tp": source}
                ).wait_recv()


def greet_all(extra, m):
    me = lax.axis_index("tp")
    barrier = pltpu.get_barrier_semaphore()
    for k in range(1, m):
        pl.semaphore_signal(
            barrier, inc=1, device_id={"tp": (me + k) % m}, device_id_type=MESH
        )
    for device in extra:
        pl.semaphore_signal(barrier, inc=1, device_id={"sp": device}, device_id_type=MESH)
    pl.semaphore_wait(barrier, m - 1 + len(extra))


def exchange_kernel(n, own, rim, out, before, send, recv, rsend, rrecv, local_sem):
    me = lax.axis_index("sp")
    barrier = pltpu.get_barrier_semaphore()
    for k in range(1, n):
        pl.semaphore_signal(
            barrier, inc=1, device_id={"sp": (me + k) % n}, device_id_type=MESH
        )
    mine = pltpu.make_async_copy(own, out.at[me], local_sem)
    mine.start()
    pl.semaphore_wait(barrier, n - 1)
    copies = [remote(rim, before, rsend, rrecv, {"sp": (me + 1) % n})]
    for k in range(1, n):
        copies.append(
            remote(own, out.at[me], send.at[k - 1], recv.at[k - 1], {"sp": (me + k) % n})
        )
    for copy in copies:
        copy.start()
    for copy in copies:
        copy.wait()
    mine.wait()


def exchange(own, rim):
    n = lax.axis_size("sp")
    return pl.pallas_call(
        functools.partial(exchange_kernel, n),
        out_shape=(
            jax.ShapeDtypeStruct((n,) + own.shape, own.dtype),
            jax.ShapeDtypeStruct(rim.shape, rim.dtype),
        ),
        in_specs=[pl.BlockSpec(memory_space=pl.ANY)] * 2,
        out_specs=(pl.BlockSpec(memory_space=pl.ANY),) * 2,
        scratch_shapes=[
            pltpu.SemaphoreType.DMA((n - 1,)),
            pltpu.SemaphoreType.DMA((n - 1,)),
            pltpu.SemaphoreType.DMA,
            pltpu.SemaphoreType.DMA,
            pltpu.SemaphoreType.DMA,
        ],
        compiler_params=pltpu.CompilerParams(collective_id=3, has_side_effects=True),
    )(own, rim)


def ring_gather(w, tok, first):
    n, m = lax.axis_size("sp"), lax.axis_size("tp")
    return pl.pallas_call(
        functools.partial(ring_kernel, n, m, first),
        out_shape=(
            jax.ShapeDtypeStruct((n,) + w.shape, w.dtype),
            jax.ShapeDtypeStruct((m,) + tok.shape, tok.dtype),
            jax.ShapeDtypeStruct((m, n // m, w.shape[0], w.shape[1] - first), w.dtype),
        ),
        in_specs=[pl.BlockSpec(memory_space=pl.ANY)] * 2,
        out_specs=(pl.BlockSpec(memory_space=pl.ANY),) * 3,
        scratch_shapes=[
            pltpu.SemaphoreType.DMA((n - 1, 2)),
            pltpu.SemaphoreType.DMA((n - 1, 2)),
            pltpu.SemaphoreType.DMA,
            pltpu.SemaphoreType.DMA((m,)),
            pltpu.SemaphoreType.DMA((m,)),
            pltpu.SemaphoreType.DMA,
            pltpu.SemaphoreType.DMA((2 * n,)),
            pltpu.SemaphoreType.DMA((m, n // m, 2)),
        ],
        compiler_params=pltpu.CompilerParams(collective_id=0, has_side_effects=True),
    )(w, tok)


def dot(a, b, dims):
    return lax.dot_general(a, b, (dims, ((), ())), preferred_element_type=jnp.float32)


def recurrence_kernel(q_ref, f_ref, i_ref, lb_ref, ds_ref, out_ref, qd_ref, st_ref, dec_ref):
    row = lax.broadcasted_iota(jnp.int32, (BLOCK, BLOCK), 0)
    col = lax.broadcasted_iota(jnp.int32, (BLOCK, BLOCK), 1)
    causal = row >= col
    lower = causal.astype(jnp.float32)
    slack = 1.0 - lb_ref[...]
    state = jnp.zeros((HEAD, HEAD), jnp.float32)
    run = jnp.zeros((1, HEAD), jnp.float32)
    for b in range(q_ref.shape[0] // BLOCK):
        rows = pl.ds(b * BLOCK, BLOCK)
        raw = q_ref[rows, :].astype(jnp.float32)
        query = raw * jax.nn.sigmoid(raw)
        gate = slack * jax.nn.sigmoid(-f_ref[rows, :].astype(jnp.float32))
        values = i_ref[rows, :]
        log_decay = jnp.log1p(-gate) + ds_ref[rows, :]
        cum = jnp.dot(
            lower, log_decay, precision=lax.Precision.HIGHEST, preferred_element_type=jnp.float32
        )
        final = cum[BLOCK - 1 :, :]
        qe = query * jnp.exp(cum)
        qb = qe.astype(jnp.bfloat16)
        ke = (gate * jnp.exp(-cum)).astype(jnp.bfloat16)
        scores = jnp.where(causal, dot(qb, ke, ((1,), (1,))), 0.0).astype(jnp.bfloat16)
        out = dot(scores, values, ((1,), (0,)))
        out_ref[rows, :] = out + dot(qb, state.astype(jnp.bfloat16), ((1,), (1,)))
        qd_ref[rows, :] = (qe * jnp.exp(run)).astype(jnp.bfloat16)
        kd = (gate * jnp.exp(final - cum)).astype(jnp.bfloat16)
        state = state * jnp.exp(final) + dot(values, kd, ((0,), (0,)))
        run = run + final
    st_ref[0] = state
    dec_ref[0] = jnp.exp(run)


def recurrence(raw, lower_bound, decay_shift, heads):
    rows = raw.shape[0]
    column = lambda k: pl.BlockSpec((rows, HEAD), lambda h: (0, k * heads + h))
    return pl.pallas_call(
        recurrence_kernel,
        grid=(heads,),
        out_shape=(
            jax.ShapeDtypeStruct((rows, heads * HEAD), jnp.float32),
            jax.ShapeDtypeStruct((rows, heads * HEAD), jnp.bfloat16),
            jax.ShapeDtypeStruct((heads, HEAD, HEAD), jnp.float32),
            jax.ShapeDtypeStruct((heads, 1, HEAD), jnp.float32),
        ),
        in_specs=[
            column(0),
            column(1),
            column(2),
            pl.BlockSpec((1, HEAD), lambda h: (0, h)),
            column(0),
        ],
        out_specs=(
            column(0),
            column(0),
            pl.BlockSpec((1, HEAD, HEAD), lambda h: (h, 0, 0)),
            pl.BlockSpec((1, 1, HEAD), lambda h: (h, 0, 0)),
        ),
    )(raw, raw, raw, lower_bound[None], decay_shift)


def local(
    tokens,
    norm_gain,
    w_query,
    w_forget,
    w_input,
    w_outgate,
    w_conv_value,
    w_conv_gate,
    w_gate_rec,
    w_gate_conv,
    lower_bound,
    decay_shift,
    state_init,
    head_gain,
    conv_kernel,
    channel_gain,
    channel_bias,
    w_out_rec,
    w_out_conv,
):
    n, m = lax.axis_size("sp"), lax.axis_size("tp")
    weights = (
        w_query,
        w_forget,
        w_input,
        w_outgate,
        w_conv_value,
        w_conv_gate,
        w_gate_rec,
        w_gate_conv,
        w_out_rec,
        w_out_conv,
    )
    width = w_query.shape[1]
    features = w_gate_rec.shape[1]
    inputs_width = 6 * width + 2 * features
    gathered, rows_all, out_w = ring_gather(
        jnp.concatenate(weights, axis=1), tokens, inputs_width
    )
    normed = normalize_rows(rows_all.reshape(-1, tokens.shape[1]), norm_gain)
    row_count = normed.shape[0]
    stacked = gathered.reshape(n * w_query.shape[0], -1)
    raw = jnp.dot(
        normed, stacked[:, :inputs_width], preferred_element_type=jnp.float32
    ).astype(jnp.bfloat16)
    share = n // m
    me = lax.axis_index("tp")
    own_w = lax.dynamic_slice_in_dim(gathered, me * share, share, 0)[:, :, inputs_width:]
    out_w = lax.dynamic_update_slice_in_dim(out_w, own_w[None], me, 0)
    out_rows, out_columns = w_out_rec.shape

    def part(k):
        return raw[:, k * width : (k + 1) * width].astype(jnp.float32)

    gated = (part(4) * jax.nn.sigmoid(part(5))).astype(jnp.bfloat16)

    heads = width // HEAD
    local_out, decayed_query, local_state, forgetting = recurrence(
        raw, lower_bound, decay_shift, heads
    )
    handover = jnp.concatenate(
        [local_state, jnp.broadcast_to(forgetting, (heads, 16, HEAD))], axis=1
    ).astype(jnp.bfloat16)
    rim_width = KW - 1
    everything, previous = exchange(handover, gated[row_count - 32 :])
    everything = everything.astype(jnp.float32)
    states, decays = everything[:, :, :HEAD], everything[:, :, HEAD : HEAD + 1]
    position = lax.axis_index("sp")
    previous = jnp.where(position > 0, previous[32 - rim_width :], 0)
    incoming = state_init.transpose(0, 2, 1)
    for k in range(n - 1):
        incoming = jnp.where(k < position, incoming * decays[k] + states[k], incoming)
    head_out = local_out.reshape(row_count, heads, HEAD) + jnp.einsum(
        "thd,hvd->thv",
        decayed_query.reshape(row_count, heads, HEAD),
        incoming.astype(jnp.bfloat16),
        preferred_element_type=jnp.float32,
    )
    head_out = head_out * lax.rsqrt(jnp.mean(head_out * head_out, axis=-1, keepdims=True) + EPSILON)
    head_out = head_out * head_gain.reshape(heads, HEAD)

    mixed_rec = (head_out.reshape(row_count, width) * jax.nn.silu(part(3))).astype(jnp.bfloat16)
    extended = jnp.concatenate([previous, gated], axis=0).astype(jnp.float32)
    conv_out = jnp.zeros((row_count, width), jnp.float32)
    for tap_index in range(KW):
        conv_out = conv_out + conv_kernel[tap_index] * extended[tap_index : tap_index + row_count]
    squares = tp_gather(jnp.sum(conv_out * conv_out, axis=1).reshape(-1, HEAD), 2)
    squares = jnp.sum(squares, axis=0).reshape(row_count)
    scale = lax.rsqrt(squares / CONV + EPSILON)[:, None]
    mixed_conv = jax.nn.silu(conv_out * scale * channel_gain + channel_bias).astype(jnp.bfloat16)

    both = tp_gather(jnp.concatenate([mixed_rec, mixed_conv], axis=1), 1, 3)

    def project(branch):
        first = branch * out_columns
        blocks = []
        for j in range(share):
            total = 0.0
            for t in range(m):
                total = total + jnp.dot(
                    both[t, :, branch * width : (branch + 1) * width],
                    out_w[t, j, :, first : first + out_columns],
                    preferred_element_type=jnp.float32,
                )
            blocks.append(total.astype(jnp.bfloat16))
        return jnp.concatenate(blocks, axis=1).astype(jnp.float32)

    gates = raw[:, 6 * width :].astype(jnp.float32)
    merged = jax.nn.sigmoid(gates[:, :features]) * project(0)
    merged = merged + jax.nn.sigmoid(gates[:, features:]) * project(1)
    return merged.astype(jnp.bfloat16)

def solution(mesh):
    in_specs = (
        P(("sp", "tp"), None),
        P(),
        P("sp", "tp"),
        P("sp", "tp"),
        P("sp", "tp"),
        P("sp", "tp"),
        P("sp", "tp"),
        P("sp", "tp"),
        P("sp", "tp"),
        P("sp", "tp"),
        P("tp"),
        P("sp", "tp"),
        P("tp", None, None),
        P("tp"),
        P(None, "tp"),
        P("tp"),
        P("tp"),
        P("tp", "sp"),
        P("tp", "sp"),
    )
    out_specs = P("sp", "tp")
    return jax.shard_map(local, mesh=mesh, in_specs=in_specs, out_specs=out_specs, check_vma=False)
```
